32 devices in a mesh: sp: 4 (over z), fs: 4 (over y, x), tp: 2 (over core).
Axes of the slice: x: 2, y: 2, z: 4, core: 2. Of those that a mesh axis runs over, the one named last changes fastest.
Arguments:
- tokens: bfloat16 [4, 512, 2048], P('fs', ('sp', 'tp')), may hold values from -6 to 6
- input_norm_gain: float32 [2048], replicated, may hold values from 0.1 to 1.9
- pooling_input_weight: bfloat16 [2048, 1024], P('sp', 'tp'), may hold values from -0.125 to 0.125
- query_weight: bfloat16 [2048, 1024], P('sp', 'tp'), may hold values from -0.125 to 0.125
- forget_weight: bfloat16 [2048, 1024], P('sp', 'tp'), may hold values from -0.125 to 0.125
- value_weight: bfloat16 [2048, 1024], P('sp', 'tp'), may hold values from -0.125 to 0.125
- pooling_group_maps: bfloat16 [4, 256, 256], P('tp'), may hold values from -0.375 to 0.375
- pooling_scale: float32 [1024], P('tp'), may hold values from 0.1 to 1.9
- lower_bound_logits: float32 [1024], P('tp')
- decay_spike: float32 [4, 512, 8], P('fs', 'sp', 'tp'), may hold values from -0.75 to 0
- head_norm_gain: float32 [1024], P('tp'), may hold values from 0.1 to 1.9
- pooling_output_weight: bfloat16 [1024, 2048], P('tp', 'sp'), may hold values from -0.125 to 0.125
- recurrent_output_weight: bfloat16 [1024, 2048], P('tp', 'sp'), may hold values from -0.125 to 0.125
Outputs:
- mixed: bfloat16 [4, 512, 2048], P('fs', ('sp', 'tp'))
The draws below stay inside these ranges and needn't reach their ends.
All inputs are finite; a program needn't handle non-finite values.
Results may differ from the reference program's by a relative error of at most 0.013.
Values may be sent and summed in bfloat16 or wider, within the bound.
A program may use at most 64 MiB of HBM per device.

```python
import jax
import jax.numpy as jnp
from jax import lax

D = 2048
POOL_GROUP = 256
POOL_GROUPS = 4
HEAD = 128
RECURRENT_HEADS = 8
BLOCK = 64
TOK_DEV = 128
D_POOL = 1024
D_REC = 1024
LEN = 512
SEQUENCE_COUNT = 4
N_TP = 2


def head_kinds(key):
    ranking = jax.random.permutation(jax.random.fold_in(key, 11), RECURRENT_HEADS)
    return ranking < RECURRENT_HEADS // 2


def draw_lower_bound_logits(key, part):
    lasting = head_kinds(key)
    spread = jax.random.uniform(jax.random.fold_in(key, 12), (RECURRENT_HEADS, HEAD), jnp.float32)
    slow_rate = 0.3 * jnp.exp(jnp.log(4.0) * spread) / LEN
    fast_rate = 0.03 * jnp.exp(jnp.log(10.0 / 3.0) * spread)
    chosen = jnp.where(lasting[:, None], slow_rate, fast_rate)
    return (jnp.log1p(-chosen) - jnp.log(chosen)).reshape(D_REC)


def draw_decay_spike(key, part):
    lasting = head_kinds(key)
    devices = LEN // TOK_DEV
    spread = jax.random.uniform(jax.random.fold_in(key, 21), (SEQUENCE_COUNT, devices, RECURRENT_HEADS), jnp.float32)
    fast_rate = 0.004 * jnp.exp(jnp.log(5.0) * spread)
    slow_rate = 0.1 * jnp.exp(jnp.log(6.0) * spread) / LEN
    local_decay_rate = jnp.repeat(jnp.where(lasting[None, None, :], slow_rate, fast_rate), TOK_DEV, axis=1)
    third_length = LEN // 3
    spike_locations = jax.random.randint(jax.random.fold_in(key, 22), (SEQUENCE_COUNT, 3, RECURRENT_HEADS), 0, third_length)
    spike_locations = spike_locations + third_length * jnp.arange(3, dtype=jnp.int32)[None, :, None]
    kept_fraction = jax.random.uniform(jax.random.fold_in(key, 23), (SEQUENCE_COUNT, 3, RECURRENT_HEADS), jnp.float32, 0.55, 0.8)
    position_index = jnp.arange(LEN, dtype=jnp.int32)
    agreement = (position_index[None, :, None, None] == spike_locations[:, None, :, :]).astype(jnp.float32)
    spikes = jnp.sum(agreement * jnp.log(kept_fraction)[:, None, :, :], axis=2)
    return spikes - local_decay_rate


def shard_levels(own_key, shape, split, smallest, largest):
    level, own = 1.0, jax.random.fold_in(own_key, 6)
    for axis_at, blocks in split:
        steps = jnp.exp(jax.random.uniform(jax.random.fold_in(own, axis_at), (blocks,), jnp.float32, smallest / len(split), largest / len(split)))
        level = level * jnp.repeat(steps, shape[axis_at] // blocks).reshape([-1 if axis == axis_at else 1 for axis in range(len(shape))])
    return level


def scatter_about(rng, dims, scale, bound, shards=(), kind=jnp.bfloat16):
    drawn = jax.random.normal(rng, dims, jnp.float32) * scale
    if len(shards) > 0:
        drawn = shard_levels(rng, dims, shards, -0.22, 0.18) * drawn
    return jnp.clip(drawn, min=-bound, max=bound).astype(kind)


def setup_inputs(seed: int = 0) -> dict:
    seeds = jax.random.split(jax.random.key(seed), 14)
    return {
        "tokens": scatter_about(seeds[0], (SEQUENCE_COUNT, LEN, D), 1.0, 6.0, ((0, 4), (1, 8))),
        "input_norm_gain": jnp.clip(1.0 + 0.18 * jax.random.normal(seeds[1], (D,), jnp.float32), 0.1, 1.9),
        "pooling_input_weight": scatter_about(seeds[2], (D, D_POOL), D ** -0.5, 0.125, ((0, 4), (1, 2))),
        "query_weight": scatter_about(seeds[3], (D, D_REC), D ** -0.5, 0.125, ((0, 4), (1, 2))),
        "forget_weight": scatter_about(seeds[4], (D, D_REC), D ** -0.5, 0.125, ((0, 4), (1, 2))),
        "value_weight": scatter_about(seeds[5], (D, D_REC), D ** -0.5, 0.125, ((0, 4), (1, 2))),
        "pooling_group_maps": scatter_about(seeds[6], (POOL_GROUPS, POOL_GROUP, POOL_GROUP), POOL_GROUP ** -0.5, 0.375, ((0, 2),)),
        "pooling_scale": jnp.clip(1.0 + 0.18 * jax.random.normal(seeds[7], (D_POOL,), jnp.float32), 0.1, 1.9),
        "lower_bound_logits": draw_lower_bound_logits(jax.random.fold_in(seeds[13], 71), 0),
        "decay_spike": draw_decay_spike(jax.random.fold_in(seeds[13], 71), 0),
        "head_norm_gain": jnp.clip(1.0 + 0.18 * jax.random.normal(seeds[10], (D_REC,), jnp.float32), 0.1, 1.9),
        "pooling_output_weight": scatter_about(seeds[11], (D_POOL, D), (D_POOL + D_REC) ** -0.5, 0.125, ((0, 2), (1, 4))),
        "recurrent_output_weight": scatter_about(seeds[12], (D_REC, D), (D_POOL + D_REC) ** -0.5, 0.125, ((0, 2), (1, 4))),
    }


EPSILON = 1e-06
HIGHEST = lax.Precision.HIGHEST

def stored(values):
    return lax.optimization_barrier(values.astype(jnp.bfloat16))

def rms_scale(values, gain):
    return values * lax.rsqrt(lax.optimization_barrier(jnp.mean(values * values, axis=-1, keepdims=True)) + EPSILON) * gain

def pooling(pool_input, pooling_group_maps, pooling_scale):
    length_total = pool_input.shape[0]
    groups = pooling_group_maps.shape[0]
    group_size = pooling_group_maps.shape[1]
    reach_rows = 2 ** groups
    padded = jnp.pad(pool_input.astype(jnp.float32).reshape(length_total, groups, group_size), ((reach_rows, 0), (0, 0), (0, 0)))
    windows = 2 ** (jnp.arange(groups, dtype=jnp.int32) + 1)
    window_sum = jnp.zeros((length_total, groups, group_size), jnp.float32)
    for offset in range(reach_rows):
        inside = (offset < windows).astype(jnp.float32)
        window_sum = window_sum + padded[reach_rows - offset:reach_rows - offset + length_total] * inside[:, None]
    counts = jnp.minimum(jnp.arange(length_total, dtype=jnp.int32)[:, None] + 1, windows[None, :]).astype(jnp.float32)
    pool_diff = stored(window_sum / counts[:, :, None] - padded[reach_rows:])
    mapped = jnp.einsum('tgc,gcd->tgd', pool_diff.astype(jnp.float32), pooling_group_maps.astype(jnp.float32))
    return (mapped.reshape(length_total, groups * group_size) * pooling_scale).astype(jnp.bfloat16)

def linear_recurrence(query_matrix, forget_gate_logit, value_projected, lower_bound_logits, spike_row, head_norm_gain):
    length_total, width = query_matrix.shape
    number_heads = spike_row.shape[1]
    head_width = width // number_heads
    block_layout = (length_total // BLOCK, BLOCK, number_heads, head_width)
    reader = jax.nn.silu(query_matrix.astype(jnp.float32)).reshape(block_layout)
    key_gate_value = jax.nn.sigmoid(-lower_bound_logits) * jax.nn.sigmoid(-forget_gate_logit.astype(jnp.float32))
    decay_logarithm = (jnp.log1p(-key_gate_value).reshape(length_total, number_heads, head_width) + spike_row[:, :, None]).reshape(block_layout)
    key_rows = key_gate_value.reshape(block_layout)
    value_rows = value_projected.astype(jnp.float32).reshape(block_layout)
    causal = (jnp.arange(BLOCK)[:, None] >= jnp.arange(BLOCK)[None, :]).astype(jnp.float32)

    def advance(carried, input_batch):
        block_reader, block_key, block_value, block_log = input_batch
        inner_log = jnp.cumsum(block_log, axis=0)
        read_scaled = block_reader * jnp.exp(inner_log)
        key_scaled = block_key * jnp.exp(-inner_log)
        scores = jnp.einsum('thd,shd->hts', read_scaled, key_scaled, precision=HIGHEST) * causal
        output = jnp.einsum('hts,she->the', scores, block_value, precision=HIGHEST)
        output = output + jnp.einsum('thd,hde->the', read_scaled, carried, precision=HIGHEST)
        closing = inner_log[-1]
        key_tail = block_key * jnp.exp(closing[None] - inner_log)
        carried = jnp.exp(closing)[:, :, None] * carried + jnp.einsum('shd,she->hde', key_tail, block_value, precision=HIGHEST)
        return (carried, output)
    initial = jnp.zeros((number_heads, head_width, head_width), jnp.float32)
    final_state, read_out = lax.scan(advance, initial, (reader, key_rows, value_rows, decay_logarithm))
    read_out = read_out.reshape(length_total, number_heads, head_width)
    return (rms_scale(read_out, 1.0).reshape(length_total, width) * head_norm_gain).astype(jnp.bfloat16)

def reference(tokens, input_norm_gain, pooling_input_weight, query_weight, forget_weight, value_weight, pooling_group_maps, pooling_scale, lower_bound_logits, decay_spike, head_norm_gain, pooling_output_weight, recurrent_output_weight):
    pool_width = pooling_input_weight.shape[1] // N_TP
    rec_width = query_weight.shape[1] // N_TP

    def sequence_tokens(input_batch):
        token_series, spike_row = input_batch
        normed = rms_scale(token_series.astype(jnp.float32), input_norm_gain).astype(jnp.bfloat16)
        pool_input = stored(jnp.dot(normed, pooling_input_weight, preferred_element_type=jnp.float32))
        query_matrix = stored(jnp.dot(normed, query_weight, preferred_element_type=jnp.float32))
        forget_gate_logit = stored(jnp.dot(normed, forget_weight, preferred_element_type=jnp.float32))
        value_projected = stored(jnp.dot(normed, value_weight, preferred_element_type=jnp.float32))
        pool_out = pooling(pool_input, pooling_group_maps, pooling_scale)
        recurrent_output = linear_recurrence(query_matrix, forget_gate_logit, value_projected, lower_bound_logits, spike_row, head_norm_gain)
        mixed_sum = jnp.zeros((token_series.shape[0], pooling_output_weight.shape[1]), jnp.float32)
        for member in range(N_TP):
            pool_lo = member * pool_width
            rec_lo = member * rec_width
            partial_value = jnp.dot(pool_out[:, pool_lo:pool_lo + pool_width], pooling_output_weight[pool_lo:pool_lo + pool_width], preferred_element_type=jnp.float32)
            partial_value = partial_value + jnp.dot(recurrent_output[:, rec_lo:rec_lo + rec_width], recurrent_output_weight[rec_lo:rec_lo + rec_width], preferred_element_type=jnp.float32)
            mixed_sum = mixed_sum + stored(partial_value).astype(jnp.float32)
        return mixed_sum.astype(jnp.bfloat16)
    return lax.map(sequence_tokens, (tokens, decay_spike))
```

```python
import functools

import jax
import jax.numpy as jnp
from jax import lax
from jax.experimental import pallas as pl
from jax.experimental.pallas import tpu as pltpu
from jax.sharding import PartitionSpec as P

BLOCK = 64


EPSILON = 1e-06
HIGHEST = lax.Precision.HIGHEST


def shifted(value, axis, steps):
    count = lax.axis_size(axis)
    first, last = (max(0, -steps), min(count, count - steps))
    return lax.ppermute(value, axis, [(source, source + steps) for source in range(first, last)])


def entering(shard, axis, join, neutral):
    place = lax.axis_index(axis)
    gathered = jax.tree.map(
        lambda a, kind: lax.all_gather(a.astype(kind), axis), shard, (jnp.bfloat16, jnp.bfloat16)
    )
    state = jax.tree.map(lambda a, e: jnp.zeros_like(a) + jnp.asarray(e, a.dtype), shard, neutral)

    def one(step, state):
        return join(
            state,
            jax.tree.map(
                lambda a, own: lax.dynamic_index_in_dim(a, step, 0, False).astype(own.dtype),
                gathered,
                shard,
            ),
        )

    return lax.fori_loop(0, place, one, state)


def rms_scale(values, gain):
    return values * lax.rsqrt(jnp.mean(values * values, axis=-1, keepdims=True) + EPSILON) * gain


def join_state(earlier, later):
    decay_one, state_one = earlier
    decay_two, state_two = later
    return (decay_one * decay_two, decay_two[..., None] * state_one + state_two)


def body(
    tokens,
    input_norm_gain,
    pooling_input_weight,
    query_weight,
    forget_weight,
    value_weight,
    pooling_group_maps,
    pooling_scale,
    lower_bound_logits,
    decay_spike,
    head_norm_gain,
    pooling_output_weight,
    recurrent_output_weight,
):
    gathered = lax.all_gather(tokens, "tp", axis=1, tiled=True)[0]
    length_total = gathered.shape[0]
    normed = rms_scale(gathered.astype(jnp.float32), input_norm_gain).astype(jnp.bfloat16)
    pool_width = pooling_input_weight.shape[1]
    rec_width = query_weight.shape[1]
    stacked = jnp.concatenate(
        [pooling_input_weight, query_weight, forget_weight, value_weight], axis=1
    )
    out_local = jnp.concatenate([pooling_output_weight, recurrent_output_weight], axis=0)
    groups_fs = lax.axis_size("fs")
    member = lax.axis_index("fs")
    slice_width = stacked.shape[1] // groups_fs
    own_slice = lax.dynamic_slice_in_dim(stacked, member * slice_width, slice_width, 1)
    column_part = lax.all_gather(own_slice, "sp", axis=0, tiled=True)
    full_input = lax.all_gather(column_part, "fs", axis=1, tiled=True)
    projected = jnp.dot(normed, full_input, preferred_element_type=jnp.float32)
    slice_height = out_local.shape[0] // groups_fs
    own_rows = lax.dynamic_slice_in_dim(out_local, member * slice_height, slice_height, 0)
    row_part = lax.all_gather(own_rows, "sp", axis=1, tiled=True)
    out_full = lax.all_gather(row_part, "fs", axis=0, tiled=True)
    rounded = lax.optimization_barrier(projected.astype(jnp.bfloat16))
    pool_input = rounded[:, :pool_width]
    query_matrix = rounded[:, pool_width : pool_width + rec_width].astype(jnp.float32)
    forget_gate_logit = rounded[:, pool_width + rec_width : pool_width + 2 * rec_width].astype(
        jnp.float32
    )
    value_projected = rounded[:, pool_width + 2 * rec_width :].astype(jnp.float32)
    groups_local = pooling_group_maps.shape[0]
    group_size = pooling_group_maps.shape[1]
    reach_rows = 2 ** (groups_local * lax.axis_size("tp"))
    previous = shifted(pool_input[length_total - reach_rows :], "sp", 1)
    extended = jnp.concatenate([previous, pool_input], axis=0).astype(jnp.float32)
    extended = extended.reshape(reach_rows + length_total, groups_local, group_size)
    group_ids = lax.axis_index("tp") * groups_local + jnp.arange(groups_local, dtype=jnp.int32)
    windows = jnp.left_shift(jnp.int32(2), group_ids)
    window_sum = jnp.zeros((length_total, groups_local, group_size), jnp.float32)
    for offset in range(reach_rows):
        inside = (offset < windows).astype(jnp.float32)
        window_sum = (
            window_sum
            + extended[reach_rows - offset : reach_rows - offset + length_total] * inside[:, None]
        )
    position_index = lax.axis_index("sp") * length_total + jnp.arange(length_total, dtype=jnp.int32)
    counts = jnp.minimum(position_index[:, None] + 1, windows[None, :]).astype(jnp.float32)
    pool_diff = (window_sum / counts[:, :, None] - extended[reach_rows:]).astype(jnp.bfloat16)
    pool_mapped = jnp.einsum(
        "tgc,gcd->tgd", pool_diff, pooling_group_maps, preferred_element_type=jnp.float32
    )
    pool_out = (pool_mapped.reshape(length_total, pool_width) * pooling_scale).astype(jnp.bfloat16)
    local_heads = decay_spike.shape[2]
    head_width = rec_width // local_heads
    blocks = length_total // BLOCK
    block_layout = (blocks, BLOCK, local_heads, head_width)
    reader = jax.nn.silu(query_matrix).reshape(block_layout)
    key_gate_value = jax.nn.sigmoid(-lower_bound_logits) * jax.nn.sigmoid(-forget_gate_logit)
    decay_logarithm = (
        jnp.log1p(-key_gate_value).reshape(length_total, local_heads, head_width)
        + decay_spike[0][:, :, None]
    ).reshape(block_layout)
    key_rows = key_gate_value.reshape(block_layout)
    value_rows = value_projected.reshape(block_layout)
    inner_log = jnp.cumsum(decay_logarithm, axis=1)
    read_scaled = reader * jnp.exp(inner_log)
    key_scaled = key_rows * jnp.exp(-inner_log)
    causal = (jnp.arange(BLOCK)[:, None] >= jnp.arange(BLOCK)[None, :]).astype(jnp.float32)
    scores = jnp.einsum("nthd,nshd->nhts", read_scaled, key_scaled, precision=HIGHEST) * causal
    within = jnp.einsum("nhts,nshe->nthe", scores, value_rows, precision=HIGHEST)
    closing = inner_log[:, -1]
    key_tail = key_rows * jnp.exp(closing[:, None] - inner_log)
    deltas = jnp.einsum("nshd,nshe->nhde", key_tail, value_rows, precision=HIGHEST)
    block_decay = jnp.exp(closing)

    def advance(carried, input_batch):
        decay_now, delta_now = input_batch
        return (decay_now[..., None] * carried + delta_now, carried)

    initial = jnp.zeros((local_heads, head_width, head_width), jnp.float32)
    device_state, entry_states = lax.scan(advance, initial, (block_decay, deltas))
    device_decay = jnp.exp(jnp.sum(closing, axis=0))
    scanned = entering(
        (device_decay, device_state),
        "sp",
        join_state,
        (jnp.ones_like(device_decay), jnp.zeros_like(device_state)),
    )
    prior_state = scanned[1]
    before = jnp.cumsum(closing, axis=0) - closing
    start_states = entry_states + jnp.exp(before)[..., None] * prior_state[None]
    read_out = within + jnp.einsum("nthd,nhde->nthe", read_scaled, start_states, precision=HIGHEST)
    read_out = read_out.reshape(length_total, local_heads, head_width)
    recurrent_output = (
        rms_scale(read_out, 1.0).reshape(length_total, rec_width) * head_norm_gain
    ).astype(jnp.bfloat16)
    mixed_rows = jnp.concatenate([pool_out, recurrent_output], axis=1)
    summed = lax.psum_scatter(
        jnp.dot(mixed_rows, out_full, preferred_element_type=jnp.float32).astype(jnp.bfloat16),
        "tp",
        scatter_dimension=0,
        tiled=True,
    )
    return summed[None]


F32 = jnp.float32
BF16 = jnp.bfloat16
NT = (((1,), (1,)), ((), ()))
TN = (((0,), (0,)), ((), ()))


def layer_kernel(
    n_sp, n_fs, n_tp,
    tok, gain, w_pool, w_query, w_forget, w_value, maps, scale, low, spike, hgain, w_po, w_ro,
    out,
    wbuf, tbuf, nbuf, sbuf, proj, pool_g, rec_g, part, dbuf, summed, obuf,
    wz_s, wz_r, wf_s, wf_r, tz_s, tz_r, td_s, td_r, ss_s, ss_r, pg_s, pg_r, rg_s, rg_r, d_s, d_r, o_s, o_r,
):
    s = lax.axis_index("sp")
    f = lax.axis_index("fs")
    t = lax.axis_index("tp")
    rows = tok.shape[0]
    depth = w_pool.shape[0]
    width = w_pool.shape[1] // n_sp
    piece = depth // n_fs
    length = n_sp * n_tp * rows
    weights = (w_pool, w_query, w_forget, w_value)

    def at(ds=0, df=0):
        return {"sp": lax.rem(s + ds, n_sp), "fs": lax.rem(f + df, n_fs), "tp": t}

    other = {"sp": s, "fs": f, "tp": 1 - t}

    def remote(src, dst, ssem, rsem, dev):
        return pltpu.make_async_remote_copy(
            src_ref=src, dst_ref=dst, send_sem=ssem, recv_sem=rsem,
            device_id=dev, device_id_type=pl.DeviceIdType.MESH,
        )

    barrier = pltpu.get_barrier_semaphore()
    partners = [at(ds=d) for d in range(1, n_sp)] + [at(df=e) for e in range(1, n_fs)] + [other]
    for dev in partners:
        pl.semaphore_signal(barrier, inc=1, device_id=dev, device_id_type=pl.DeviceIdType.MESH)
    pl.semaphore_wait(barrier, len(partners))

    def weight_copy(d, m):
        dest = lax.rem(s + d, n_sp)
        src = weights[m].at[pl.ds(pl.multiple_of(f * piece, piece), piece), pl.ds(pl.multiple_of(dest * width, width), width)]
        dst = wbuf.at[pl.ds(pl.multiple_of(s * depth + f * piece, piece), piece), pl.ds(m * width, width)]
        return remote(src, dst, wz_s.at[d - 1, m], wz_r.at[d - 1, m], at(ds=d))

    def weight_pass(d, e):
        origin = lax.rem(s - d + n_sp, n_sp)
        view = wbuf.at[pl.ds(pl.multiple_of(origin * depth + f * piece, piece), piece), :]
        return remote(view, view, wf_s.at[d - 1, e - 1], wf_r.at[d - 1, e - 1], at(df=e))

    def weight_received(d, e):
        origin = lax.rem(s - d + n_sp, n_sp)
        giver = lax.rem(f - e + n_fs, n_fs)
        view = wbuf.at[pl.ds(pl.multiple_of(origin * depth + giver * piece, piece), piece), :]
        return remote(view, view, wf_s.at[d - 1, e - 1], wf_r.at[d - 1, e - 1], at(df=e))

    def weight_arrival(d, m):
        origin = lax.rem(s - d + n_sp, n_sp)
        dst = wbuf.at[pl.ds(pl.multiple_of(origin * depth + f * piece, piece), piece), pl.ds(m * width, width)]
        return remote(dst, dst, wz_s.at[d - 1, m], wz_r.at[d - 1, m], at(ds=d))

    def spike_copy(d):
        dest = lax.rem(s + d, n_sp)
        return remote(spike.at[dest], sbuf.at[s], ss_s.at[d - 1], ss_r.at[d - 1], at(ds=d))

    def line(own, slots, send_sems, recv_sems):
        def sending(way, k):
            step = 1 - 2 * way
            origin = s - step * k
            dst = slots(origin)
            src = own if k == 0 else dst
            return remote(src, dst, send_sems.at[way, k], recv_sems.at[way, k], at(ds=step + n_sp))

        def arriving(way, k):
            step = 1 - 2 * way
            dst = slots(s - step * (k + 1))
            return remote(dst, dst, send_sems.at[way, k], recv_sems.at[way, k], at(ds=step + n_sp))

        def can_send(way, k):
            if way == 0:
                return jnp.logical_and(s - k >= 0, s + 1 < n_sp)
            return jnp.logical_and(s + k < n_sp, s - 1 >= 0)

        def will_arrive(way, k):
            return s - (k + 1) >= 0 if way == 0 else s + (k + 1) < n_sp

        return sending, arriving, can_send, will_arrive

    def hop_start(parts, k):
        sending, _, can_send, _ = parts
        for way in (0, 1):
            @pl.when(can_send(way, k))
            def _(way=way):
                sending(way, k).start()

    def hop_finish(parts):
        sending, _, can_send, _ = parts
        for k in range(n_sp - 1):
            for way in (0, 1):
                @pl.when(can_send(way, k))
                def _(way=way, k=k):
                    sending(way, k).wait_send()

    for d in (1, 3, 2) if n_sp == 4 else range(1, n_sp):
        for m in range(4):
            weight_copy(d, m).start()
    tokens_line = line(tok, lambda o: tbuf.at[o, t], tz_s, tz_r)
    hop_start(tokens_line, 0)
    own_pass = remote(tok, tbuf.at[s, t], td_s.at[s], td_r.at[s], other)
    own_pass.start()
    for d in range(1, n_sp):
        spike_copy(d).start()

    def core_pass(origin):
        view = tbuf.at[origin, t]
        return remote(view, view, td_s.at[origin], td_r.at[origin], other)

    def core_arrival(origin):
        view = tbuf.at[origin, 1 - t]
        return remote(view, view, td_s.at[origin], td_r.at[origin], other)

    gain_row = gain[...]

    def normalise(values, origin, core):
        x = values.astype(F32)
        y = x * lax.rsqrt(jnp.mean(x * x, axis=-1, keepdims=True) + EPSILON) * gain_row
        nbuf[origin, core] = y.astype(BF16)

    for m in range(4):
        wbuf[pl.ds(pl.multiple_of(s * depth, depth), depth), m * width:(m + 1) * width] = weights[m][
            :, pl.ds(pl.multiple_of(s * width, width), width)
        ]
    sbuf[s] = spike[s]
    normalise(tok[...], s, t)

    order = (1, 3, 2) if n_sp == 4 else tuple(range(1, n_sp))
    for k in range(n_sp - 1):
        for way in (0, 1):
            @pl.when(tokens_line[3](way, k))
            def _(way=way, k=k):
                tokens_line[1](way, k).wait_recv()
                if k + 1 < n_sp - 1:
                    @pl.when(tokens_line[2](way, k + 1))
                    def _():
                        tokens_line[0](way, k + 1).start()
                core_pass(s - (1 - 2 * way) * (k + 1)).start()
        d = order[k]
        for m in range(4):
            weight_arrival(d, m).wait_recv()
        for e in range(1, n_fs):
            weight_pass(d, e).start()
        for way in (0, 1):
            @pl.when(tokens_line[3](way, k))
            def _(way=way, k=k):
                origin = s - (1 - 2 * way) * (k + 1)
                normalise(tbuf[origin, t], origin, t)

    @pl.loop(0, n_sp)
    def _(origin):
        core_arrival(origin).wait_recv()
        normalise(tbuf[origin, 1 - t], origin, 1 - t)

    for d in order:
        for e in range(1, n_fs):
            weight_received(d, e).wait_recv()
    for d in range(1, n_sp):
        dst = sbuf.at[lax.rem(s - d + n_sp, n_sp)]
        remote(dst, dst, ss_s.at[d - 1], ss_r.at[d - 1], at(ds=d)).wait_recv()

    @pl.loop(0, n_sp)
    def _(origin):
        x = nbuf[origin].reshape(n_tp * rows, nbuf.shape[3])
        proj[origin] = jnp.dot(x, wbuf[...], preferred_element_type=F32).astype(BF16)

    projected = proj[...].reshape(length, 4 * width)
    x = projected[:, :width].astype(F32)
    group_size = maps.shape[1]
    groups = maps.shape[0]
    share = group_size // width
    group = t * groups + s // share
    position = lax.broadcasted_iota(jnp.int32, (length, width), 0)
    total = x
    window_sum = x
    window = jnp.int32(2)
    for g in range(n_tp * groups):
        reach = 2 ** g
        total = total + jnp.concatenate([jnp.zeros((reach, width), F32), total[: length - reach]], axis=0)
        window_sum = total if g == 0 else jnp.where(group == g, total, window_sum)
    for g in range(1, n_tp * groups):
        window = jnp.where(group == g, 2 ** (g + 1), window)
    counts = jnp.minimum(position + 1, window).astype(F32)
    pool_g[s] = (window_sum / counts - x).astype(BF16)
    pool_line = line(pool_g.at[s], lambda o: pool_g.at[o], pg_s, pg_r)
    hop_start(pool_line, 0)

    lows = low[s]
    tri_r = lax.broadcasted_iota(jnp.int32, (BLOCK, BLOCK), 0)
    tri_c = lax.broadcasted_iota(jnp.int32, (BLOCK, BLOCK), 1)
    causal = tri_r >= tri_c
    tri = causal.astype(F32)
    gate_low = jax.nn.sigmoid(-lows)
    state = jnp.zeros((width, width), F32)
    per_origin = length // n_sp
    columns = [jnp.transpose(sbuf[o])[:, :1] for o in range(n_sp)]
    for b in range(length // BLOCK):
        lo = b * BLOCK
        here = slice(lo, lo + BLOCK)
        q = projected[here, width:2 * width].astype(F32)
        logit = projected[here, 2 * width:3 * width].astype(F32)
        v = projected[here, 3 * width:]
        reader = q * jax.nn.sigmoid(q)
        key = gate_low * jax.nn.sigmoid(-logit)
        off = lo % per_origin
        logs = jnp.log1p(-key) + columns[lo // per_origin][off:off + BLOCK]
        inner = jnp.dot(tri, logs, preferred_element_type=F32, precision=HIGHEST)
        read_scaled = (reader * jnp.exp(inner)).astype(BF16)
        key_scaled = (key * jnp.exp(-inner)).astype(BF16)
        scores = lax.dot_general(read_scaled, key_scaled, NT, preferred_element_type=F32)
        scores = jnp.where(causal, scores, 0.0).astype(BF16)
        read = jnp.dot(scores, v, preferred_element_type=F32)
        read = read + lax.dot_general(read_scaled, state.astype(BF16), NT, preferred_element_type=F32)
        closing = inner[BLOCK - 1:]
        key_tail = (key * jnp.exp(closing - inner)).astype(BF16)
        state = jnp.exp(closing) * state + lax.dot_general(v, key_tail, TN, preferred_element_type=F32)
        rec = read * lax.rsqrt(jnp.mean(read * read, axis=-1, keepdims=True) + EPSILON) * hgain[s]
        rec_g[s, lo:lo + BLOCK] = rec.astype(BF16)
    rec_line = line(rec_g.at[s], lambda o: rec_g.at[o], rg_s, rg_r)
    hop_start(rec_line, 0)

    for k in range(n_sp - 1):
        for parts in (pool_line, rec_line):
            for way in (0, 1):
                @pl.when(parts[3](way, k))
                def _(way=way, k=k, parts=parts):
                    parts[1](way, k).wait_recv()
                    if k + 1 < n_sp - 1:
                        @pl.when(parts[2](way, k + 1))
                        def _():
                            parts[0](way, k + 1).start()

    strip = n_tp * rows
    @pl.loop(0, n_sp)
    def _(o):
        here = pl.ds(pl.multiple_of(o * strip, strip), strip)
        mixed_row = []
        for g in range(groups):
            diff = jnp.concatenate([pool_g[g * share + c, here] for c in range(share)], axis=1)
            mapped = jnp.dot(diff, maps[g], preferred_element_type=F32)
            mixed_row.append((mapped * scale[:, g * group_size:(g + 1) * group_size]).astype(BF16))
        acc = jnp.dot(jnp.concatenate(mixed_row, axis=1), w_po[...], preferred_element_type=F32)
        recs = jnp.concatenate([rec_g[c, here] for c in range(n_sp)], axis=1)
        acc = acc + jnp.dot(recs, w_ro[...], preferred_element_type=F32)
        acc = acc.astype(BF16)
        for core in range(n_tp):
            part[core, o] = acc[core * rows:(core + 1) * rows]

    across = remote(part.at[1 - t], dbuf, d_s, d_r, other)
    across.start()
    across.wait_recv()
    summed[...] = (part[t].astype(F32) + dbuf[...].astype(F32)).astype(BF16)

    def out_copy(d):
        dest = lax.rem(s + d, n_sp)
        return remote(summed.at[dest], obuf.at[s], o_s.at[d - 1], o_r.at[d - 1], at(ds=d))

    for d in order:
        out_copy(d).start()
    obuf[s] = summed[s]
    for d in order:
        dst = obuf.at[lax.rem(s - d + n_sp, n_sp)]
        remote(dst, dst, o_s.at[d - 1], o_r.at[d - 1], at(ds=d)).wait_recv()
    cols = w_po.shape[1]
    for o in range(n_sp):
        out[:, o * cols:(o + 1) * cols] = obuf[o]

    for d in range(1, n_sp):
        for m in range(4):
            weight_copy(d, m).wait_send()
        for e in range(1, n_fs):
            weight_pass(d, e).wait_send()
        spike_copy(d).wait_send()
        out_copy(d).wait_send()
    hop_finish(tokens_line)
    hop_finish(pool_line)
    hop_finish(rec_line)
    own_pass.wait_send()
    for k in range(n_sp - 1):
        for way in (0, 1):
            @pl.when(tokens_line[3](way, k))
            def _(way=way, k=k):
                core_pass(s - (1 - 2 * way) * (k + 1)).wait_send()
    across.wait_send()


def head_body(sizes, *args):
    (tokens, gain, w_pool, w_query, w_forget, w_value, maps, scale, low, spike, hgain, w_po, w_ro) = args
    n_sp, n_fs, n_tp = sizes
    tok = tokens[0]
    rows, features = tok.shape
    width = w_pool.shape[1] // n_sp
    length = n_sp * n_tp * rows
    cols = w_po.shape[1]
    spikes = jnp.broadcast_to(spike[0].T[:, None, :], (spike.shape[2], 8, spike.shape[1]))
    dma = pltpu.SemaphoreType.DMA
    whole = pl.BlockSpec(memory_space=pltpu.VMEM)
    hop = (2, n_sp - 1)
    result = pl.pallas_call(
        functools.partial(layer_kernel, n_sp, n_fs, n_tp),
        out_shape=jax.ShapeDtypeStruct((rows, n_sp * cols), BF16),
        in_specs=[whole] * 13,
        out_specs=whole,
        scratch_shapes=[
            pltpu.VMEM((features, 4 * width), BF16),
            pltpu.VMEM((n_sp, n_tp, rows, features), BF16),
            pltpu.VMEM((n_sp, n_tp, rows, features), BF16),
            pltpu.VMEM((n_sp, 8, spike.shape[1]), F32),
            pltpu.VMEM((n_sp, n_tp * rows, 4 * width), BF16),
            pltpu.VMEM((n_sp, length, width), BF16),
            pltpu.VMEM((n_sp, length, width), BF16),
            pltpu.VMEM((n_tp, n_sp, rows, cols), BF16),
            pltpu.VMEM((n_sp, rows, cols), BF16),
            pltpu.VMEM((n_sp, rows, cols), BF16),
            pltpu.VMEM((n_sp, rows, cols), BF16),
            dma((n_sp - 1, 4)), dma((n_sp - 1, 4)),
            dma((n_sp - 1, n_fs - 1)), dma((n_sp - 1, n_fs - 1)),
            dma(hop), dma(hop),
            dma((n_sp,)), dma((n_sp,)),
            dma((n_sp - 1,)), dma((n_sp - 1,)),
            dma(hop), dma(hop),
            dma(hop), dma(hop),
            dma, dma,
            dma((n_sp - 1,)), dma((n_sp - 1,)),
        ],
        compiler_params=pltpu.CompilerParams(
            collective_id=0, has_side_effects=True, vmem_limit_bytes=56 * 1024 * 1024
        ),
        name="layer",
    )(
        tok, gain[None], w_pool, w_query, w_forget, w_value, maps, scale[None],
        low.reshape(n_sp, 1, width), spikes, hgain.reshape(n_sp, 1, width), w_po, w_ro,
    )
    return result[None]


def solution(mesh):
    placed = (
        P("fs", ("sp", "tp"), None),
        P(),
        P("sp", "tp"),
        P("sp", "tp"),
        P("sp", "tp"),
        P("sp", "tp"),
        P("tp", None, None),
        P("tp"),
        P("tp"),
        P("fs", "sp", "tp"),
        P("tp"),
        P("tp", "sp"),
        P("tp", "sp"),
    )
    sizes = (mesh.shape["sp"], mesh.shape["fs"], mesh.shape["tp"])

    def one(*args):
        maps, spike = args[6], args[9]
        width = args[2].shape[1] // sizes[0]
        fits = spike.shape[2] == sizes[0] and sizes[2] == 2 and width % 128 == 0
        fits = fits and args[3].shape[1] == args[2].shape[1] and maps.shape[1] % width == 0
        return head_body(sizes, *args) if fits else body(*args)

    return jax.shard_map(
        one, mesh=mesh, in_specs=placed, out_specs=P("fs", ("sp", "tp"), None), check_vma=False
    )
```

```python
import functools

import jax
import jax.numpy as jnp
from jax import lax
from jax.experimental import pallas as pl
from jax.experimental.pallas import tpu as pltpu
from jax.sharding import PartitionSpec as P

BLOCK = 64


EPSILON = 1e-06
HIGHEST = lax.Precision.HIGHEST


def shifted(value, axis, steps):
    count = lax.axis_size(axis)
    first, last = (max(0, -steps), min(count, count - steps))
    return lax.ppermute(value, axis, [(source, source + steps) for source in range(first, last)])


def entering(shard, axis, join, neutral):
    place = lax.axis_index(axis)
    gathered = jax.tree.map(
        lambda a, kind: lax.all_gather(a.astype(kind), axis), shard, (jnp.bfloat16, jnp.bfloat16)
    )
    state = jax.tree.map(lambda a, e: jnp.zeros_like(a) + jnp.asarray(e, a.dtype), shard, neutral)

    def one(step, state):
        return join(
            state,
            jax.tree.map(
                lambda a, own: lax.dynamic_index_in_dim(a, step, 0, False).astype(own.dtype),
                gathered,
                shard,
            ),
        )

    return lax.fori_loop(0, place, one, state)


def rms_scale(values, gain):
    return values * lax.rsqrt(jnp.mean(values * values, axis=-1, keepdims=True) + EPSILON) * gain


def join_state(earlier, later):
    decay_one, state_one = earlier
    decay_two, state_two = later
    return (decay_one * decay_two, decay_two[..., None] * state_one + state_two)


def body(
    tokens,
    input_norm_gain,
    pooling_input_weight,
    query_weight,
    forget_weight,
    value_weight,
    pooling_group_maps,
    pooling_scale,
    lower_bound_logits,
    decay_spike,
    head_norm_gain,
    pooling_output_weight,
    recurrent_output_weight,
):
    gathered = lax.all_gather(tokens, "tp", axis=1, tiled=True)[0]
    length_total = gathered.shape[0]
    normed = rms_scale(gathered.astype(jnp.float32), input_norm_gain).astype(jnp.bfloat16)
    pool_width = pooling_input_weight.shape[1]
    rec_width = query_weight.shape[1]
    stacked = jnp.concatenate(
        [pooling_input_weight, query_weight, forget_weight, value_weight], axis=1
    )
    out_local = jnp.concatenate([pooling_output_weight, recurrent_output_weight], axis=0)
    groups_fs = lax.axis_size("fs")
    member = lax.axis_index("fs")
    slice_width = stacked.shape[1] // groups_fs
    own_slice = lax.dynamic_slice_in_dim(stacked, member * slice_width, slice_width, 1)
    column_part = lax.all_gather(own_slice, "sp", axis=0, tiled=True)
    full_input = lax.all_gather(column_part, "fs", axis=1, tiled=True)
    projected = jnp.dot(normed, full_input, preferred_element_type=jnp.float32)
    slice_height = out_local.shape[0] // groups_fs
    own_rows = lax.dynamic_slice_in_dim(out_local, member * slice_height, slice_height, 0)
    row_part = lax.all_gather(own_rows, "sp", axis=1, tiled=True)
    out_full = lax.all_gather(row_part, "fs", axis=0, tiled=True)
    rounded = lax.optimization_barrier(projected.astype(jnp.bfloat16))
    pool_input = rounded[:, :pool_width]
    query_matrix = rounded[:, pool_width : pool_width + rec_width].astype(jnp.float32)
    forget_gate_logit = rounded[:, pool_width + rec_width : pool_width + 2 * rec_width].astype(
        jnp.float32
    )
    value_projected = rounded[:, pool_width + 2 * rec_width :].astype(jnp.float32)
    groups_local = pooling_group_maps.shape[0]
    group_size = pooling_group_maps.shape[1]
    reach_rows = 2 ** (groups_local * lax.axis_size("tp"))
    previous = shifted(pool_input[length_total - reach_rows :], "sp", 1)
    extended = jnp.concatenate([previous, pool_input], axis=0).astype(jnp.float32)
    extended = extended.reshape(reach_rows + length_total, groups_local, group_size)
    group_ids = lax.axis_index("tp") * groups_local + jnp.arange(groups_local, dtype=jnp.int32)
    windows = jnp.left_shift(jnp.int32(2), group_ids)
    window_sum = jnp.zeros((length_total, groups_local, group_size), jnp.float32)
    for offset in range(reach_rows):
        inside = (offset < windows).astype(jnp.float32)
        window_sum = (
            window_sum
            + extended[reach_rows - offset : reach_rows - offset + length_total] * inside[:, None]
        )
    position_index = lax.axis_index("sp") * length_total + jnp.arange(length_total, dtype=jnp.int32)
    counts = jnp.minimum(position_index[:, None] + 1, windows[None, :]).astype(jnp.float32)
    pool_diff = (window_sum / counts[:, :, None] - extended[reach_rows:]).astype(jnp.bfloat16)
    pool_mapped = jnp.einsum(
        "tgc,gcd->tgd", pool_diff, pooling_group_maps, preferred_element_type=jnp.float32
    )
    pool_out = (pool_mapped.reshape(length_total, pool_width) * pooling_scale).astype(jnp.bfloat16)
    local_heads = decay_spike.shape[2]
    head_width = rec_width // local_heads
    blocks = length_total // BLOCK
    block_layout = (blocks, BLOCK, local_heads, head_width)
    reader = jax.nn.silu(query_matrix).reshape(block_layout)
    key_gate_value = jax.nn.sigmoid(-lower_bound_logits) * jax.nn.sigmoid(-forget_gate_logit)
    decay_logarithm = (
        jnp.log1p(-key_gate_value).reshape(length_total, local_heads, head_width)
        + decay_spike[0][:, :, None]
    ).reshape(block_layout)
    key_rows = key_gate_value.reshape(block_layout)
    value_rows = value_projected.reshape(block_layout)
    inner_log = jnp.cumsum(decay_logarithm, axis=1)
    read_scaled = reader * jnp.exp(inner_log)
    key_scaled = key_rows * jnp.exp(-inner_log)
    causal = (jnp.arange(BLOCK)[:, None] >= jnp.arange(BLOCK)[None, :]).astype(jnp.float32)
    scores = jnp.einsum("nthd,nshd->nhts", read_scaled, key_scaled, precision=HIGHEST) * causal
    within = jnp.einsum("nhts,nshe->nthe", scores, value_rows, precision=HIGHEST)
    closing = inner_log[:, -1]
    key_tail = key_rows * jnp.exp(closing[:, None] - inner_log)
    deltas = jnp.einsum("nshd,nshe->nhde", key_tail, value_rows, precision=HIGHEST)
    block_decay = jnp.exp(closing)

    def advance(carried, input_batch):
        decay_now, delta_now = input_batch
        return (decay_now[..., None] * carried + delta_now, carried)

    initial = jnp.zeros((local_heads, head_width, head_width), jnp.float32)
    device_state, entry_states = lax.scan(advance, initial, (block_decay, deltas))
    device_decay = jnp.exp(jnp.sum(closing, axis=0))
    scanned = entering(
        (device_decay, device_state),
        "sp",
        join_state,
        (jnp.ones_like(device_decay), jnp.zeros_like(device_state)),
    )
    prior_state = scanned[1]
    before = jnp.cumsum(closing, axis=0) - closing
    start_states = entry_states + jnp.exp(before)[..., None] * prior_state[None]
    read_out = within + jnp.einsum("nthd,nhde->nthe", read_scaled, start_states, precision=HIGHEST)
    read_out = read_out.reshape(length_total, local_heads, head_width)
    recurrent_output = (
        rms_scale(read_out, 1.0).reshape(length_total, rec_width) * head_norm_gain
    ).astype(jnp.bfloat16)
    mixed_rows = jnp.concatenate([pool_out, recurrent_output], axis=1)
    summed = lax.psum_scatter(
        jnp.dot(mixed_rows, out_full, preferred_element_type=jnp.float32).astype(jnp.bfloat16),
        "tp",
        scatter_dimension=0,
        tiled=True,
    )
    return summed[None]


F32 = jnp.float32
BF16 = jnp.bfloat16
NT = (((1,), (1,)), ((), ()))
TN = (((0,), (0,)), ((), ()))


def layer_kernel(
    n_sp, n_fs, n_tp,
    tok, gain, w_pool, w_query, w_forget, w_value, maps, scale, low, spike, hgain, w_po, w_ro,
    out,
    wbuf, tbuf, nbuf, sbuf, proj, pool_g, rec_g, part, dbuf, summed, obuf,
    wz_s, wz_r, wf_s, wf_r, tz_s, tz_r, td_s, td_r, ss_s, ss_r, pg_s, pg_r, rg_s, rg_r, d_s, d_r, o_s, o_r,
):
    s = lax.axis_index("sp")
    f = lax.axis_index("fs")
    t = lax.axis_index("tp")
    rows = tok.shape[0]
    depth = w_pool.shape[0]
    width = w_pool.shape[1] // n_sp
    piece = depth // n_fs
    length = n_sp * n_tp * rows
    weights = (w_pool, w_query, w_forget, w_value)

    def at(ds=0, df=0):
        return {"sp": lax.rem(s + ds, n_sp), "fs": lax.rem(f + df, n_fs), "tp": t}

    other = {"sp": s, "fs": f, "tp": 1 - t}

    def remote(src, dst, ssem, rsem, dev):
        return pltpu.make_async_remote_copy(
            src_ref=src, dst_ref=dst, send_sem=ssem, recv_sem=rsem,
            device_id=dev, device_id_type=pl.DeviceIdType.MESH,
        )

    barrier = pltpu.get_barrier_semaphore()
    partners = [at(ds=d) for d in range(1, n_sp)] + [at(df=e) for e in range(1, n_fs)] + [other]
    for dev in partners:
        pl.semaphore_signal(barrier, inc=1, device_id=dev, device_id_type=pl.DeviceIdType.MESH)
    pl.semaphore_wait(barrier, len(partners))

    def weight_copy(d, m):
        dest = lax.rem(s + d, n_sp)
        src = weights[m].at[pl.ds(pl.multiple_of(f * piece, piece), piece), pl.ds(pl.multiple_of(dest * width, width), width)]
        dst = wbuf.at[pl.ds(pl.multiple_of(s * depth + f * piece, piece), piece), pl.ds(m * width, width)]
        return remote(src, dst, wz_s.at[d - 1, m], wz_r.at[d - 1, m], at(ds=d))

    def weight_pass(d, e):
        origin = lax.rem(s - d + n_sp, n_sp)
        view = wbuf.at[pl.ds(pl.multiple_of(origin * depth + f * piece, piece), piece), :]
        return remote(view, view, wf_s.at[d - 1, e - 1], wf_r.at[d - 1, e - 1], at(df=e))

    def weight_received(d, e):
        origin = lax.rem(s - d + n_sp, n_sp)
        giver = lax.rem(f - e + n_fs, n_fs)
        view = wbuf.at[pl.ds(pl.multiple_of(origin * depth + giver * piece, piece), piece), :]
        return remote(view, view, wf_s.at[d - 1, e - 1], wf_r.at[d - 1, e - 1], at(df=e))

    def weight_arrival(d, m):
        origin = lax.rem(s - d + n_sp, n_sp)
        dst = wbuf.at[pl.ds(pl.multiple_of(origin * depth + f * piece, piece), piece), pl.ds(m * width, width)]
        return remote(dst, dst, wz_s.at[d - 1, m], wz_r.at[d - 1, m], at(ds=d))

    def spike_copy(d):
        dest = lax.rem(s + d, n_sp)
        return remote(spike.at[dest], sbuf.at[s], ss_s.at[d - 1], ss_r.at[d - 1], at(ds=d))

    def line(own, slots, send_sems, recv_sems):
        def sending(way, k):
            step = 1 - 2 * way
            origin = s - step * k
            dst = slots(origin)
            src = own if k == 0 else dst
            return remote(src, dst, send_sems.at[way, k], recv_sems.at[way, k], at(ds=step + n_sp))

        def arriving(way, k):
            step = 1 - 2 * way
            dst = slots(s - step * (k + 1))
            return remote(dst, dst, send_sems.at[way, k], recv_sems.at[way, k], at(ds=step + n_sp))

        def can_send(way, k):
            if way == 0:
                return jnp.logical_and(s - k >= 0, s + 1 < n_sp)
            return jnp.logical_and(s + k < n_sp, s - 1 >= 0)

        def will_arrive(way, k):
            return s - (k + 1) >= 0 if way == 0 else s + (k + 1) < n_sp

        return sending, arriving, can_send, will_arrive

    def hop_start(parts, k):
        sending, _, can_send, _ = parts
        for way in (0, 1):
            @pl.when(can_send(way, k))
            def _(way=way):
                sending(way, k).start()

    def hop_finish(parts):
        sending, _, can_send, _ = parts
        for k in range(n_sp - 1):
            for way in (0, 1):
                @pl.when(can_send(way, k))
                def _(way=way, k=k):
                    sending(way, k).wait_send()

    for d in (1, 3, 2) if n_sp == 4 else range(1, n_sp):
        for m in range(4):
            weight_copy(d, m).start()
    tokens_line = line(tok, lambda o: tbuf.at[o, t], tz_s, tz_r)
    hop_start(tokens_line, 0)
    own_pass = remote(tok, tbuf.at[s, t], td_s.at[s], td_r.at[s], other)
    own_pass.start()
    for d in range(1, n_sp):
        spike_copy(d).start()

    def core_pass(origin):
        view = tbuf.at[origin, t]
        return remote(view, view, td_s.at[origin], td_r.at[origin], other)

    def core_arrival(origin):
        view = tbuf.at[origin, 1 - t]
        return remote(view, view, td_s.at[origin], td_r.at[origin], other)

    gain_row = gain[...]

    def normalise(values, origin, core):
        x = values.astype(F32)
        y = x * lax.rsqrt(jnp.mean(x * x, axis=-1, keepdims=True) + EPSILON) * gain_row
        nbuf[origin, core] = y.astype(BF16)

    for m in range(4):
        wbuf[pl.ds(pl.multiple_of(s * depth, depth), depth), m * width:(m + 1) * width] = weights[m][
            :, pl.ds(pl.multiple_of(s * width, width), width)
        ]
    sbuf[s] = spike[s]
    normalise(tok[...], s, t)

    order = (1, 3, 2) if n_sp == 4 else tuple(range(1, n_sp))
    for d in order:
        for m in range(4):
            weight_arrival(d, m).wait_recv()
        for e in range(1, n_fs):
            weight_pass(d, e).start()
    for k in range(n_sp - 1):
        for way in (0, 1):
            @pl.when(tokens_line[3](way, k))
            def _(way=way, k=k):
                origin = s - (1 - 2 * way) * (k + 1)
                tokens_line[1](way, k).wait_recv()
                if k + 1 < n_sp - 1:
                    @pl.when(tokens_line[2](way, k + 1))
                    def _():
                        tokens_line[0](way, k + 1).start()
                core_pass(origin).start()
        for way in (0, 1):
            @pl.when(tokens_line[3](way, k))
            def _(way=way, k=k):
                origin = s - (1 - 2 * way) * (k + 1)
                normalise(tbuf[origin, t], origin, t)

    @pl.loop(0, n_sp)
    def _(origin):
        core_arrival(origin).wait_recv()
        normalise(tbuf[origin, 1 - t], origin, 1 - t)

    for d in order:
        for e in range(1, n_fs):
            weight_received(d, e).wait_recv()
    for d in range(1, n_sp):
        dst = sbuf.at[lax.rem(s - d + n_sp, n_sp)]
        remote(dst, dst, ss_s.at[d - 1], ss_r.at[d - 1], at(ds=d)).wait_recv()

    tall = max(1, n_sp // 2)
    @pl.loop(0, n_sp // tall)
    def _(i):
        x = nbuf[pl.ds(i * tall, tall)].reshape(tall * n_tp * rows, nbuf.shape[3])
        y = jnp.dot(x, wbuf[...], preferred_element_type=F32).astype(BF16)
        proj[pl.ds(i * tall, tall)] = y.reshape(tall, n_tp * rows, 4 * width)

    projected = proj[...].reshape(length, 4 * width)
    x = projected[:, :width].astype(F32)
    group_size = maps.shape[1]
    groups = maps.shape[0]
    share = group_size // width
    group = t * groups + s // share
    position = lax.broadcasted_iota(jnp.int32, (length, width), 0)
    total = x
    window_sum = x
    window = jnp.int32(2)
    for g in range(n_tp * groups):
        reach = 2 ** g
        total = total + jnp.concatenate([jnp.zeros((reach, width), F32), total[: length - reach]], axis=0)
        window_sum = total if g == 0 else jnp.where(group == g, total, window_sum)
    for g in range(1, n_tp * groups):
        window = jnp.where(group == g, 2 ** (g + 1), window)
    counts = jnp.minimum(position + 1, window).astype(F32)
    pool_g[s] = (window_sum / counts - x).astype(BF16)
    pool_line = line(pool_g.at[s], lambda o: pool_g.at[o], pg_s, pg_r)
    hop_start(pool_line, 0)

    lows = low[s]
    tri_r = lax.broadcasted_iota(jnp.int32, (BLOCK, BLOCK), 0)
    tri_c = lax.broadcasted_iota(jnp.int32, (BLOCK, BLOCK), 1)
    causal = tri_r >= tri_c
    tri = causal.astype(F32)
    gate_low = jax.nn.sigmoid(-lows)
    state = jnp.zeros((width, width), F32)
    per_origin = length // n_sp
    columns = [jnp.transpose(sbuf[o])[:, :1] for o in range(n_sp)]
    for b in range(length // BLOCK):
        lo = b * BLOCK
        here = slice(lo, lo + BLOCK)
        q = projected[here, width:2 * width].astype(F32)
        logit = projected[here, 2 * width:3 * width].astype(F32)
        v = projected[here, 3 * width:]
        reader = q * jax.nn.sigmoid(q)
        key = gate_low * jax.nn.sigmoid(-logit)
        off = lo % per_origin
        logs = jnp.log1p(-key) + columns[lo // per_origin][off:off + BLOCK]
        inner = jnp.dot(tri, logs, preferred_element_type=F32, precision=HIGHEST)
        read_scaled = (reader * jnp.exp(inner)).astype(BF16)
        key_scaled = (key * jnp.exp(-inner)).astype(BF16)
        scores = lax.dot_general(read_scaled, key_scaled, NT, preferred_element_type=F32)
        scores = jnp.where(causal, scores, 0.0).astype(BF16)
        read = jnp.dot(scores, v, preferred_element_type=F32)
        read = read + lax.dot_general(read_scaled, state.astype(BF16), NT, preferred_element_type=F32)
        closing = inner[BLOCK - 1:]
        key_tail = (key * jnp.exp(closing - inner)).astype(BF16)
        state = jnp.exp(closing) * state + lax.dot_general(v, key_tail, TN, preferred_element_type=F32)
        rec = read * lax.rsqrt(jnp.mean(read * read, axis=-1, keepdims=True) + EPSILON) * hgain[s]
        rec_g[s, lo:lo + BLOCK] = rec.astype(BF16)
    strip = n_tp * rows
    strips = (0, 3, 1, 2) if n_sp == 4 else tuple(range(n_sp))

    def strip_line(p):
        here = pl.ds(p * strip, strip)
        return line(rec_g.at[s, here], lambda o: rec_g.at[o, here], rg_s.at[p], rg_r.at[p])

    rec_lines = [strip_line(p) for p in range(n_sp)]
    for p in strips:
        hop_start(rec_lines[p], 0)

    def relay(parts, k):
        for way in (0, 1):
            @pl.when(parts[3](way, k))
            def _(way=way):
                parts[1](way, k).wait_recv()
                if k + 1 < n_sp - 1:
                    @pl.when(parts[2](way, k + 1))
                    def _():
                        parts[0](way, k + 1).start()

    def across(p):
        return remote(part.at[1 - t, p], dbuf.at[p], d_s.at[p], d_r.at[p], other)

    def out_copy(p):
        return remote(summed.at[p], obuf.at[s], o_s.at[p], o_r.at[s], {"sp": p, "fs": f, "tp": t})

    def settle(p):
        across(p).wait_recv()
        summed[p] = (part[t, p].astype(F32) + dbuf[p].astype(F32)).astype(BF16)

        @pl.when(s != p)
        def _():
            out_copy(p).start()

        @pl.when(s == p)
        def _():
            obuf[p] = summed[p]

    for k in range(n_sp - 1):
        relay(pool_line, k)
        if k < n_sp - 2:
            for p in strips:
                relay(rec_lines[p], k)

    def project(p):
        here = slice(p * strip, (p + 1) * strip)
        mixed_row = []
        for g in range(groups):
            diff = jnp.concatenate([pool_g[g * share + c, here] for c in range(share)], axis=1)
            mapped = jnp.dot(diff, maps[g], preferred_element_type=F32)
            mixed_row.append((mapped * scale[:, g * group_size:(g + 1) * group_size]).astype(BF16))
        acc = jnp.dot(jnp.concatenate(mixed_row, axis=1), w_po[...], preferred_element_type=F32)
        recs = jnp.concatenate([rec_g[c, here] for c in range(n_sp)], axis=1)
        acc = acc + jnp.dot(recs, w_ro[...], preferred_element_type=F32)
        acc = acc.astype(BF16)
        for core in range(n_tp):
            part[core, p] = acc[core * rows:(core + 1) * rows]
        across(p).start()

    before = None
    for p in strips:
        relay(rec_lines[p], n_sp - 2)
        project(p)
        if before is not None:
            settle(before)
        before = p
    settle(before)

    for d in order:
        origin = lax.rem(s + d, n_sp)
        dst = obuf.at[origin]
        remote(dst, dst, o_s.at[origin], o_r.at[origin], at(ds=d)).wait_recv()
    cols = w_po.shape[1]
    for o in range(n_sp):
        out[:, o * cols:(o + 1) * cols] = obuf[o]

    for d in range(1, n_sp):
        for m in range(4):
            weight_copy(d, m).wait_send()
        for e in range(1, n_fs):
            weight_pass(d, e).wait_send()
        spike_copy(d).wait_send()
    hop_finish(tokens_line)
    hop_finish(pool_line)
    for p in range(n_sp):
        hop_finish(rec_lines[p])
        across(p).wait_send()

        @pl.when(s != p)
        def _(p=p):
            out_copy(p).wait_send()
    own_pass.wait_send()
    for k in range(n_sp - 1):
        for way in (0, 1):
            @pl.when(tokens_line[3](way, k))
            def _(way=way, k=k):
                core_pass(s - (1 - 2 * way) * (k + 1)).wait_send()


def head_body(sizes, *args):
    (tokens, gain, w_pool, w_query, w_forget, w_value, maps, scale, low, spike, hgain, w_po, w_ro) = args
    n_sp, n_fs, n_tp = sizes
    tok = tokens[0]
    rows, features = tok.shape
    width = w_pool.shape[1] // n_sp
    length = n_sp * n_tp * rows
    cols = w_po.shape[1]
    spikes = jnp.broadcast_to(spike[0].T[:, None, :], (spike.shape[2], 8, spike.shape[1]))
    dma = pltpu.SemaphoreType.DMA
    whole = pl.BlockSpec(memory_space=pltpu.VMEM)
    hop = (2, n_sp - 1)
    result = pl.pallas_call(
        functools.partial(layer_kernel, n_sp, n_fs, n_tp),
        out_shape=jax.ShapeDtypeStruct((rows, n_sp * cols), BF16),
        in_specs=[whole] * 13,
        out_specs=whole,
        scratch_shapes=[
            pltpu.VMEM((features, 4 * width), BF16),
            pltpu.VMEM((n_sp, n_tp, rows, features), BF16),
            pltpu.VMEM((n_sp, n_tp, rows, features), BF16),
            pltpu.VMEM((n_sp, 8, spike.shape[1]), F32),
            pltpu.VMEM((n_sp, n_tp * rows, 4 * width), BF16),
            pltpu.VMEM((n_sp, length, width), BF16),
            pltpu.VMEM((n_sp, length, width), BF16),
            pltpu.VMEM((n_tp, n_sp, rows, cols), BF16),
            pltpu.VMEM((n_sp, rows, cols), BF16),
            pltpu.VMEM((n_sp, rows, cols), BF16),
            pltpu.VMEM((n_sp, rows, cols), BF16),
            dma((n_sp - 1, 4)), dma((n_sp - 1, 4)),
            dma((n_sp - 1, n_fs - 1)), dma((n_sp - 1, n_fs - 1)),
            dma(hop), dma(hop),
            dma((n_sp,)), dma((n_sp,)),
            dma((n_sp - 1,)), dma((n_sp - 1,)),
            dma(hop), dma(hop),
            dma((n_sp,) + hop), dma((n_sp,) + hop),
            dma((n_sp,)), dma((n_sp,)),
            dma((n_sp,)), dma((n_sp,)),
        ],
        compiler_params=pltpu.CompilerParams(
            collective_id=0, has_side_effects=True, vmem_limit_bytes=56 * 1024 * 1024
        ),
        name="layer",
    )(
        tok, gain[None], w_pool, w_query, w_forget, w_value, maps, scale[None],
        low.reshape(n_sp, 1, width), spikes, hgain.reshape(n_sp, 1, width), w_po, w_ro,
    )
    return result[None]


def solution(mesh):
    placed = (
        P("fs", ("sp", "tp"), None),
        P(),
        P("sp", "tp"),
        P("sp", "tp"),
        P("sp", "tp"),
        P("sp", "tp"),
        P("tp", None, None),
        P("tp"),
        P("tp"),
        P("fs", "sp", "tp"),
        P("tp"),
        P("tp", "sp"),
        P("tp", "sp"),
    )
    sizes = (mesh.shape["sp"], mesh.shape["fs"], mesh.shape["tp"])

    def one(*args):
        maps, spike = args[6], args[9]
        width = args[2].shape[1] // sizes[0]
        fits = spike.shape[2] == sizes[0] and sizes[2] == 2 and width % 128 == 0
        fits = fits and args[3].shape[1] == args[2].shape[1] and maps.shape[1] % width == 0
        return head_body(sizes, *args) if fits else body(*args)

    return jax.shard_map(
        one, mesh=mesh, in_specs=placed, out_specs=P("fs", ("sp", "tp"), None), check_vma=False
    )
```

```python
import functools

import jax
import jax.numpy as jnp
from jax import lax
from jax.experimental import pallas as pl
from jax.experimental.pallas import tpu as pltpu
from jax.sharding import PartitionSpec as P

BLOCK = 64


EPSILON = 1e-06
HIGHEST = lax.Precision.HIGHEST


def shifted(value, axis, steps):
    count = lax.axis_size(axis)
    first, last = (max(0, -steps), min(count, count - steps))
    return lax.ppermute(value, axis, [(source, source + steps) for source in range(first, last)])


def entering(shard, axis, join, neutral):
    place = lax.axis_index(axis)
    gathered = jax.tree.map(
        lambda a, kind: lax.all_gather(a.astype(kind), axis), shard, (jnp.bfloat16, jnp.bfloat16)
    )
    state = jax.tree.map(lambda a, e: jnp.zeros_like(a) + jnp.asarray(e, a.dtype), shard, neutral)

    def one(step, state):
        return join(
            state,
            jax.tree.map(
                lambda a, own: lax.dynamic_index_in_dim(a, step, 0, False).astype(own.dtype),
                gathered,
                shard,
            ),
        )

    return lax.fori_loop(0, place, one, state)


def rms_scale(values, gain):
    return values * lax.rsqrt(jnp.mean(values * values, axis=-1, keepdims=True) + EPSILON) * gain


def join_state(earlier, later):
    decay_one, state_one = earlier
    decay_two, state_two = later
    return (decay_one * decay_two, decay_two[..., None] * state_one + state_two)


def body(
    tokens,
    input_norm_gain,
    pooling_input_weight,
    query_weight,
    forget_weight,
    value_weight,
    pooling_group_maps,
    pooling_scale,
    lower_bound_logits,
    decay_spike,
    head_norm_gain,
    pooling_output_weight,
    recurrent_output_weight,
):
    gathered = lax.all_gather(tokens, "tp", axis=1, tiled=True)[0]
    length_total = gathered.shape[0]
    normed = rms_scale(gathered.astype(jnp.float32), input_norm_gain).astype(jnp.bfloat16)
    pool_width = pooling_input_weight.shape[1]
    rec_width = query_weight.shape[1]
    stacked = jnp.concatenate(
        [pooling_input_weight, query_weight, forget_weight, value_weight], axis=1
    )
    out_local = jnp.concatenate([pooling_output_weight, recurrent_output_weight], axis=0)
    groups_fs = lax.axis_size("fs")
    member = lax.axis_index("fs")
    slice_width = stacked.shape[1] // groups_fs
    own_slice = lax.dynamic_slice_in_dim(stacked, member * slice_width, slice_width, 1)
    column_part = lax.all_gather(own_slice, "sp", axis=0, tiled=True)
    full_input = lax.all_gather(column_part, "fs", axis=1, tiled=True)
    projected = jnp.dot(normed, full_input, preferred_element_type=jnp.float32)
    slice_height = out_local.shape[0] // groups_fs
    own_rows = lax.dynamic_slice_in_dim(out_local, member * slice_height, slice_height, 0)
    row_part = lax.all_gather(own_rows, "sp", axis=1, tiled=True)
    out_full = lax.all_gather(row_part, "fs", axis=0, tiled=True)
    rounded = lax.optimization_barrier(projected.astype(jnp.bfloat16))
    pool_input = rounded[:, :pool_width]
    query_matrix = rounded[:, pool_width : pool_width + rec_width].astype(jnp.float32)
    forget_gate_logit = rounded[:, pool_width + rec_width : pool_width + 2 * rec_width].astype(
        jnp.float32
    )
    value_projected = rounded[:, pool_width + 2 * rec_width :].astype(jnp.float32)
    groups_local = pooling_group_maps.shape[0]
    group_size = pooling_group_maps.shape[1]
    reach_rows = 2 ** (groups_local * lax.axis_size("tp"))
    previous = shifted(pool_input[length_total - reach_rows :], "sp", 1)
    extended = jnp.concatenate([previous, pool_input], axis=0).astype(jnp.float32)
    extended = extended.reshape(reach_rows + length_total, groups_local, group_size)
    group_ids = lax.axis_index("tp") * groups_local + jnp.arange(groups_local, dtype=jnp.int32)
    windows = jnp.left_shift(jnp.int32(2), group_ids)
    window_sum = jnp.zeros((length_total, groups_local, group_size), jnp.float32)
    for offset in range(reach_rows):
        inside = (offset < windows).astype(jnp.float32)
        window_sum = (
            window_sum
            + extended[reach_rows - offset : reach_rows - offset + length_total] * inside[:, None]
        )
    position_index = lax.axis_index("sp") * length_total + jnp.arange(length_total, dtype=jnp.int32)
    counts = jnp.minimum(position_index[:, None] + 1, windows[None, :]).astype(jnp.float32)
    pool_diff = (window_sum / counts[:, :, None] - extended[reach_rows:]).astype(jnp.bfloat16)
    pool_mapped = jnp.einsum(
        "tgc,gcd->tgd", pool_diff, pooling_group_maps, preferred_element_type=jnp.float32
    )
    pool_out = (pool_mapped.reshape(length_total, pool_width) * pooling_scale).astype(jnp.bfloat16)
    local_heads = decay_spike.shape[2]
    head_width = rec_width // local_heads
    blocks = length_total // BLOCK
    block_layout = (blocks, BLOCK, local_heads, head_width)
    reader = jax.nn.silu(query_matrix).reshape(block_layout)
    key_gate_value = jax.nn.sigmoid(-lower_bound_logits) * jax.nn.sigmoid(-forget_gate_logit)
    decay_logarithm = (
        jnp.log1p(-key_gate_value).reshape(length_total, local_heads, head_width)
        + decay_spike[0][:, :, None]
    ).reshape(block_layout)
    key_rows = key_gate_value.reshape(block_layout)
    value_rows = value_projected.reshape(block_layout)
    inner_log = jnp.cumsum(decay_logarithm, axis=1)
    read_scaled = reader * jnp.exp(inner_log)
    key_scaled = key_rows * jnp.exp(-inner_log)
    causal = (jnp.arange(BLOCK)[:, None] >= jnp.arange(BLOCK)[None, :]).astype(jnp.float32)
    scores = jnp.einsum("nthd,nshd->nhts", read_scaled, key_scaled, precision=HIGHEST) * causal
    within = jnp.einsum("nhts,nshe->nthe", scores, value_rows, precision=HIGHEST)
    closing = inner_log[:, -1]
    key_tail = key_rows * jnp.exp(closing[:, None] - inner_log)
    deltas = jnp.einsum("nshd,nshe->nhde", key_tail, value_rows, precision=HIGHEST)
    block_decay = jnp.exp(closing)

    def advance(carried, input_batch):
        decay_now, delta_now = input_batch
        return (decay_now[..., None] * carried + delta_now, carried)

    initial = jnp.zeros((local_heads, head_width, head_width), jnp.float32)
    device_state, entry_states = lax.scan(advance, initial, (block_decay, deltas))
    device_decay = jnp.exp(jnp.sum(closing, axis=0))
    scanned = entering(
        (device_decay, device_state),
        "sp",
        join_state,
        (jnp.ones_like(device_decay), jnp.zeros_like(device_state)),
    )
    prior_state = scanned[1]
    before = jnp.cumsum(closing, axis=0) - closing
    start_states = entry_states + jnp.exp(before)[..., None] * prior_state[None]
    read_out = within + jnp.einsum("nthd,nhde->nthe", read_scaled, start_states, precision=HIGHEST)
    read_out = read_out.reshape(length_total, local_heads, head_width)
    recurrent_output = (
        rms_scale(read_out, 1.0).reshape(length_total, rec_width) * head_norm_gain
    ).astype(jnp.bfloat16)
    mixed_rows = jnp.concatenate([pool_out, recurrent_output], axis=1)
    summed = lax.psum_scatter(
        jnp.dot(mixed_rows, out_full, preferred_element_type=jnp.float32).astype(jnp.bfloat16),
        "tp",
        scatter_dimension=0,
        tiled=True,
    )
    return summed[None]


F32 = jnp.float32
BF16 = jnp.bfloat16
NT = (((1,), (1,)), ((), ()))
TN = (((0,), (0,)), ((), ()))


def layer_kernel(
    n_sp, n_fs, n_tp,
    tok, gain, w_pool, w_query, w_forget, w_value, maps, scale, low, spike, hgain, w_po, w_ro,
    out,
    wbuf, tbuf, nbuf, sbuf, proj, pool_g, rec_g, part, dbuf, summed, obuf,
    wz_s, wz_r, wf_s, wf_r, tz_s, tz_r, td_s, td_r, ss_s, ss_r, pg_s, pg_r, rg_s, rg_r, d_s, d_r, o_s, o_r,
):
    s = lax.axis_index("sp")
    f = lax.axis_index("fs")
    t = lax.axis_index("tp")
    rows = tok.shape[0]
    depth = w_pool.shape[0]
    width = w_pool.shape[1] // n_sp
    piece = depth // n_fs
    length = n_sp * n_tp * rows
    weights = (w_pool, w_query, w_forget, w_value)

    def at(ds=0, df=0):
        return {"sp": lax.rem(s + ds, n_sp), "fs": lax.rem(f + df, n_fs), "tp": t}

    other = {"sp": s, "fs": f, "tp": 1 - t}

    def remote(src, dst, ssem, rsem, dev):
        return pltpu.make_async_remote_copy(
            src_ref=src, dst_ref=dst, send_sem=ssem, recv_sem=rsem,
            device_id=dev, device_id_type=pl.DeviceIdType.MESH,
        )

    barrier = pltpu.get_barrier_semaphore()
    partners = [at(ds=d) for d in range(1, n_sp)] + [at(df=e) for e in range(1, n_fs)] + [other]
    for dev in partners:
        pl.semaphore_signal(barrier, inc=1, device_id=dev, device_id_type=pl.DeviceIdType.MESH)
    pl.semaphore_wait(barrier, len(partners))

    def weight_copy(d, m):
        dest = lax.rem(s + d, n_sp)
        src = weights[m].at[pl.ds(pl.multiple_of(f * piece, piece), piece), pl.ds(pl.multiple_of(dest * width, width), width)]
        dst = wbuf.at[pl.ds(pl.multiple_of(s * depth + f * piece, piece), piece), pl.ds(m * width, width)]
        return remote(src, dst, wz_s.at[d - 1, m], wz_r.at[d - 1, m], at(ds=d))

    def weight_pass(d, e):
        origin = lax.rem(s - d + n_sp, n_sp)
        view = wbuf.at[pl.ds(pl.multiple_of(origin * depth + f * piece, piece), piece), :]
        return remote(view, view, wf_s.at[d - 1, e - 1], wf_r.at[d - 1, e - 1], at(df=e))

    def weight_received(d, e):
        origin = lax.rem(s - d + n_sp, n_sp)
        giver = lax.rem(f - e + n_fs, n_fs)
        view = wbuf.at[pl.ds(pl.multiple_of(origin * depth + giver * piece, piece), piece), :]
        return remote(view, view, wf_s.at[d - 1, e - 1], wf_r.at[d - 1, e - 1], at(df=e))

    def weight_arrival(d, m):
        origin = lax.rem(s - d + n_sp, n_sp)
        dst = wbuf.at[pl.ds(pl.multiple_of(origin * depth + f * piece, piece), piece), pl.ds(m * width, width)]
        return remote(dst, dst, wz_s.at[d - 1, m], wz_r.at[d - 1, m], at(ds=d))

    def spike_copy(d):
        dest = lax.rem(s + d, n_sp)
        return remote(spike.at[dest], sbuf.at[s], ss_s.at[d - 1], ss_r.at[d - 1], at(ds=d))

    def line(own, slots, send_sems, recv_sems):
        def sending(way, k):
            step = 1 - 2 * way
            origin = s - step * k
            dst = slots(origin)
            src = own if k == 0 else dst
            return remote(src, dst, send_sems.at[way, k], recv_sems.at[way, k], at(ds=step + n_sp))

        def arriving(way, k):
            step = 1 - 2 * way
            dst = slots(s - step * (k + 1))
            return remote(dst, dst, send_sems.at[way, k], recv_sems.at[way, k], at(ds=step + n_sp))

        def can_send(way, k):
            if way == 0:
                return jnp.logical_and(s - k >= 0, s + 1 < n_sp)
            return jnp.logical_and(s + k < n_sp, s - 1 >= 0)

        def will_arrive(way, k):
            return s - (k + 1) >= 0 if way == 0 else s + (k + 1) < n_sp

        return sending, arriving, can_send, will_arrive

    def hop_start(parts, k):
        sending, _, can_send, _ = parts
        for way in (0, 1):
            @pl.when(can_send(way, k))
            def _(way=way):
                sending(way, k).start()

    def hop_finish(parts):
        sending, _, can_send, _ = parts
        for k in range(n_sp - 1):
            for way in (0, 1):
                @pl.when(can_send(way, k))
                def _(way=way, k=k):
                    sending(way, k).wait_send()

    for d in (1, 3, 2) if n_sp == 4 else range(1, n_sp):
        for m in range(4):
            weight_copy(d, m).start()
    tokens_line = line(tok, lambda o: tbuf.at[o, t], tz_s, tz_r)
    hop_start(tokens_line, 0)
    own_pass = remote(tok, tbuf.at[s, t], td_s.at[s], td_r.at[s], other)
    own_pass.start()
    for d in range(1, n_sp):
        spike_copy(d).start()

    def core_pass(origin):
        view = tbuf.at[origin, t]
        return remote(view, view, td_s.at[origin], td_r.at[origin], other)

    def core_arrival(origin):
        view = tbuf.at[origin, 1 - t]
        return remote(view, view, td_s.at[origin], td_r.at[origin], other)

    gain_row = gain[...]

    def normalise(values, origin, core):
        x = values.astype(F32)
        y = x * lax.rsqrt(jnp.mean(x * x, axis=-1, keepdims=True) + EPSILON) * gain_row
        nbuf[origin, core] = y.astype(BF16)

    for m in range(4):
        wbuf[pl.ds(pl.multiple_of(s * depth, depth), depth), m * width:(m + 1) * width] = weights[m][
            :, pl.ds(pl.multiple_of(s * width, width), width)
        ]
    sbuf[s] = spike[s]
    normalise(tok[...], s, t)

    order = (1, 3, 2) if n_sp == 4 else tuple(range(1, n_sp))
    for d in order:
        for m in range(4):
            weight_arrival(d, m).wait_recv()
        for e in range(1, n_fs):
            weight_pass(d, e).start()
    def token_hop(k):
        for way in (0, 1):
            @pl.when(tokens_line[3](way, k))
            def _(way=way):
                origin = s - (1 - 2 * way) * (k + 1)
                tokens_line[1](way, k).wait_recv()
                if k + 1 < n_sp - 1:
                    @pl.when(tokens_line[2](way, k + 1))
                    def _():
                        tokens_line[0](way, k + 1).start()
                core_pass(origin).start()
        for way in (0, 1):
            @pl.when(tokens_line[3](way, k))
            def _(way=way):
                origin = s - (1 - 2 * way) * (k + 1)
                normalise(tbuf[origin, t], origin, t)

    def finish(origin):
        core_arrival(origin).wait_recv()
        normalise(tbuf[origin, 1 - t], origin, 1 - t)
        x = nbuf[origin].reshape(n_tp * rows, nbuf.shape[3])
        proj[origin] = jnp.dot(x, wbuf[...], preferred_element_type=F32).astype(BF16)

    for k in range(n_sp - 2):
        token_hop(k)
    for d in order:
        for e in range(1, n_fs):
            weight_received(d, e).wait_recv()
    for d in range(1, n_sp):
        dst = sbuf.at[lax.rem(s - d + n_sp, n_sp)]
        remote(dst, dst, ss_s.at[d - 1], ss_r.at[d - 1], at(ds=d)).wait_recv()

    near_low = jnp.maximum(s - (n_sp - 2), 0)
    near_high = jnp.minimum(s + (n_sp - 2), n_sp - 1)

    @pl.loop(0, n_sp)
    def _(origin):
        @pl.when(jnp.logical_and(origin >= near_low, origin <= near_high))
        def _():
            finish(origin)

    if n_sp > 1:
        token_hop(n_sp - 2)
    for way in (0, 1):
        @pl.when(tokens_line[3](way, n_sp - 2))
        def _(way=way):
            finish(s - (1 - 2 * way) * (n_sp - 1))

    projected = proj[...].reshape(length, 4 * width)
    x = projected[:, :width].astype(F32)
    group_size = maps.shape[1]
    groups = maps.shape[0]
    share = group_size // width
    group = t * groups + s // share
    position = lax.broadcasted_iota(jnp.int32, (length, width), 0)
    total = x
    window_sum = x
    window = jnp.int32(2)
    for g in range(n_tp * groups):
        reach = 2 ** g
        total = total + jnp.concatenate([jnp.zeros((reach, width), F32), total[: length - reach]], axis=0)
        window_sum = total if g == 0 else jnp.where(group == g, total, window_sum)
    for g in range(1, n_tp * groups):
        window = jnp.where(group == g, 2 ** (g + 1), window)
    counts = jnp.minimum(position + 1, window).astype(F32)
    pool_g[s] = (window_sum / counts - x).astype(BF16)
    pool_line = line(pool_g.at[s], lambda o: pool_g.at[o], pg_s, pg_r)
    hop_start(pool_line, 0)

    lows = low[s]
    tri_r = lax.broadcasted_iota(jnp.int32, (BLOCK, BLOCK), 0)
    tri_c = lax.broadcasted_iota(jnp.int32, (BLOCK, BLOCK), 1)
    causal = tri_r >= tri_c
    tri = causal.astype(F32)
    gate_low = jax.nn.sigmoid(-lows)
    state = jnp.zeros((width, width), F32)
    per_origin = length // n_sp
    columns = [jnp.transpose(sbuf[o])[:, :1] for o in range(n_sp)]
    for b in range(length // BLOCK):
        lo = b * BLOCK
        here = slice(lo, lo + BLOCK)
        q = projected[here, width:2 * width].astype(F32)
        logit = projected[here, 2 * width:3 * width].astype(F32)
        v = projected[here, 3 * width:]
        reader = q * jax.nn.sigmoid(q)
        key = gate_low * jax.nn.sigmoid(-logit)
        off = lo % per_origin
        logs = jnp.log1p(-key) + columns[lo // per_origin][off:off + BLOCK]
        inner = jnp.dot(tri, logs, preferred_element_type=F32, precision=HIGHEST)
        read_scaled = (reader * jnp.exp(inner)).astype(BF16)
        key_scaled = (key * jnp.exp(-inner)).astype(BF16)
        scores = lax.dot_general(read_scaled, key_scaled, NT, preferred_element_type=F32)
        scores = jnp.where(causal, scores, 0.0).astype(BF16)
        read = jnp.dot(scores, v, preferred_element_type=F32)
        read = read + lax.dot_general(read_scaled, state.astype(BF16), NT, preferred_element_type=F32)
        closing = inner[BLOCK - 1:]
        key_tail = (key * jnp.exp(closing - inner)).astype(BF16)
        state = jnp.exp(closing) * state + lax.dot_general(v, key_tail, TN, preferred_element_type=F32)
        rec = read * lax.rsqrt(jnp.mean(read * read, axis=-1, keepdims=True) + EPSILON) * hgain[s]
        rec_g[s, lo:lo + BLOCK] = rec.astype(BF16)
    strip = n_tp * rows
    strips = (0, 3, 1, 2) if n_sp == 4 else tuple(range(n_sp))

    def strip_line(p):
        here = pl.ds(p * strip, strip)
        return line(rec_g.at[s, here], lambda o: rec_g.at[o, here], rg_s.at[p], rg_r.at[p])

    rec_lines = [strip_line(p) for p in range(n_sp)]
    for p in strips:
        hop_start(rec_lines[p], 0)

    def relay(parts, k):
        for way in (0, 1):
            @pl.when(parts[3](way, k))
            def _(way=way):
                parts[1](way, k).wait_recv()
                if k + 1 < n_sp - 1:
                    @pl.when(parts[2](way, k + 1))
                    def _():
                        parts[0](way, k + 1).start()

    def across(p):
        return remote(part.at[1 - t, p], dbuf.at[p], d_s.at[p], d_r.at[p], other)

    def out_copy(p):
        return remote(summed.at[p], obuf.at[s], o_s.at[p], o_r.at[s], {"sp": p, "fs": f, "tp": t})

    def settle(p):
        across(p).wait_recv()
        summed[p] = (part[t, p].astype(F32) + dbuf[p].astype(F32)).astype(BF16)

        @pl.when(s != p)
        def _():
            out_copy(p).start()

        @pl.when(s == p)
        def _():
            obuf[p] = summed[p]

    for k in range(n_sp - 1):
        relay(pool_line, k)
        if k < n_sp - 2:
            for p in strips:
                relay(rec_lines[p], k)

    def project(p):
        here = slice(p * strip, (p + 1) * strip)
        mixed_row = []
        for g in range(groups):
            diff = jnp.concatenate([pool_g[g * share + c, here] for c in range(share)], axis=1)
            mapped = jnp.dot(diff, maps[g], preferred_element_type=F32)
            mixed_row.append((mapped * scale[:, g * group_size:(g + 1) * group_size]).astype(BF16))
        acc = jnp.dot(jnp.concatenate(mixed_row, axis=1), w_po[...], preferred_element_type=F32)
        recs = jnp.concatenate([rec_g[c, here] for c in range(n_sp)], axis=1)
        acc = acc + jnp.dot(recs, w_ro[...], preferred_element_type=F32)
        acc = acc.astype(BF16)
        for core in range(n_tp):
            part[core, p] = acc[core * rows:(core + 1) * rows]
        across(p).start()

    before = None
    for p in strips:
        relay(rec_lines[p], n_sp - 2)
        project(p)
        if before is not None:
            settle(before)
        before = p
    settle(before)

    for d in order:
        origin = lax.rem(s + d, n_sp)
        dst = obuf.at[origin]
        remote(dst, dst, o_s.at[origin], o_r.at[origin], at(ds=d)).wait_recv()
    cols = w_po.shape[1]
    for o in range(n_sp):
        out[:, o * cols:(o + 1) * cols] = obuf[o]

    for d in range(1, n_sp):
        for m in range(4):
            weight_copy(d, m).wait_send()
        for e in range(1, n_fs):
            weight_pass(d, e).wait_send()
        spike_copy(d).wait_send()
    hop_finish(tokens_line)
    hop_finish(pool_line)
    for p in range(n_sp):
        hop_finish(rec_lines[p])
        across(p).wait_send()

        @pl.when(s != p)
        def _(p=p):
            out_copy(p).wait_send()
    own_pass.wait_send()
    for k in range(n_sp - 1):
        for way in (0, 1):
            @pl.when(tokens_line[3](way, k))
            def _(way=way, k=k):
                core_pass(s - (1 - 2 * way) * (k + 1)).wait_send()


def head_body(sizes, *args):
    (tokens, gain, w_pool, w_query, w_forget, w_value, maps, scale, low, spike, hgain, w_po, w_ro) = args
    n_sp, n_fs, n_tp = sizes
    tok = tokens[0]
    rows, features = tok.shape
    width = w_pool.shape[1] // n_sp
    length = n_sp * n_tp * rows
    cols = w_po.shape[1]
    spikes = jnp.broadcast_to(spike[0].T[:, None, :], (spike.shape[2], 8, spike.shape[1]))
    dma = pltpu.SemaphoreType.DMA
    whole = pl.BlockSpec(memory_space=pltpu.VMEM)
    hop = (2, n_sp - 1)
    result = pl.pallas_call(
        functools.partial(layer_kernel, n_sp, n_fs, n_tp),
        out_shape=jax.ShapeDtypeStruct((rows, n_sp * cols), BF16),
        in_specs=[whole] * 13,
        out_specs=whole,
        scratch_shapes=[
            pltpu.VMEM((features, 4 * width), BF16),
            pltpu.VMEM((n_sp, n_tp, rows, features), BF16),
            pltpu.VMEM((n_sp, n_tp, rows, features), BF16),
            pltpu.VMEM((n_sp, 8, spike.shape[1]), F32),
            pltpu.VMEM((n_sp, n_tp * rows, 4 * width), BF16),
            pltpu.VMEM((n_sp, length, width), BF16),
            pltpu.VMEM((n_sp, length, width), BF16),
            pltpu.VMEM((n_tp, n_sp, rows, cols), BF16),
            pltpu.VMEM((n_sp, rows, cols), BF16),
            pltpu.VMEM((n_sp, rows, cols), BF16),
            pltpu.VMEM((n_sp, rows, cols), BF16),
            dma((n_sp - 1, 4)), dma((n_sp - 1, 4)),
            dma((n_sp - 1, n_fs - 1)), dma((n_sp - 1, n_fs - 1)),
            dma(hop), dma(hop),
            dma((n_sp,)), dma((n_sp,)),
            dma((n_sp - 1,)), dma((n_sp - 1,)),
            dma(hop), dma(hop),
            dma((n_sp,) + hop), dma((n_sp,) + hop),
            dma((n_sp,)), dma((n_sp,)),
            dma((n_sp,)), dma((n_sp,)),
        ],
        compiler_params=pltpu.CompilerParams(
            collective_id=0, has_side_effects=True, vmem_limit_bytes=56 * 1024 * 1024
        ),
        name="layer",
    )(
        tok, gain[None], w_pool, w_query, w_forget, w_value, maps, scale[None],
        low.reshape(n_sp, 1, width), spikes, hgain.reshape(n_sp, 1, width), w_po, w_ro,
    )
    return result[None]


def solution(mesh):
    placed = (
        P("fs", ("sp", "tp"), None),
        P(),
        P("sp", "tp"),
        P("sp", "tp"),
        P("sp", "tp"),
        P("sp", "tp"),
        P("tp", None, None),
        P("tp"),
        P("tp"),
        P("fs", "sp", "tp"),
        P("tp"),
        P("tp", "sp"),
        P("tp", "sp"),
    )
    sizes = (mesh.shape["sp"], mesh.shape["fs"], mesh.shape["tp"])

    def one(*args):
        maps, spike = args[6], args[9]
        width = args[2].shape[1] // sizes[0]
        fits = spike.shape[2] == sizes[0] and sizes[2] == 2 and width % 128 == 0
        fits = fits and args[3].shape[1] == args[2].shape[1] and maps.shape[1] % width == 0
        return head_body(sizes, *args) if fits else body(*args)

    return jax.shard_map(
        one, mesh=mesh, in_specs=placed, out_specs=P("fs", ("sp", "tp"), None), check_vma=False
    )
```
